32 devices in a mesh: sp: 8 (over z, y), tp: 4 (over x, core).
Axes of the slice: x: 2, y: 2, z: 4, core: 2. Of those that a mesh axis runs over, the one named last changes fastest.
Arguments:
- conv_input: bfloat16 [4096, 1024], P('sp', 'tp'), may hold values from -6 to 6
- gate_inner: bfloat16 [4096, 1024], P('sp', 'tp'), may hold values from -6 to 6
- gate_outer: bfloat16 [4096, 1024], P('sp', 'tp'), may hold values from -6 to 6
- conv_taps: bfloat16 [3, 1024], P(None, 'tp'), may hold values from -3.5 to 3.5
- doc_ids: int32 [4096], P('sp'), may hold values from 0 to 3, never falling along the last dimension, each value on 1 to 2048 neighbouring positions
- residual_in: bfloat16 [4096, 2048], P(('sp', 'tp')), may hold values from -6 to 6
- out_proj: bfloat16 [1024, 2048], replicated, may hold values from -0.1875 to 0.1875
- norm_gain: float32 [2048], replicated, may hold values from 0.1 to 1.9
- expert_ids: int32 [4096, 2], P(('sp', 'tp')), may hold values from 0 to 31, all different within a row; in each aligned block of 128 rows (0 to 127, 128 to 255, ...) at most 16 rows name the same one
- expert_weights: float32 [4096, 2], P(('sp', 'tp')), may hold values from 0.2 to 1
- gate_proj: bfloat16 [32, 2048, 1024], P(('sp', 'tp')), may hold values from -0.125 to 0.125
- up_proj: bfloat16 [32, 2048, 1024], P(('sp', 'tp')), may hold values from -0.125 to 0.125
- down_proj: bfloat16 [32, 1024, 2048], P(('sp', 'tp')), may hold values from -0.1875 to 0.1875
Outputs:
- layer_out: bfloat16 [4096, 2048], P(('sp', 'tp'))
The draws below stay inside these ranges and needn't reach their ends.
Inputs may be any that keep to these rules, and one draw needn't show every extreme that they name: `doc_ids`: never falls along positions; each document has at most 2048 positions. `expert_ids`: each row names 2 different experts; within the rows of one device, aligned blocks of 128 rows, no expert is named more than 16 times, a bound that some block reaches.
All inputs are finite; a program needn't handle non-finite values.
Results may differ from the reference program's by a relative error of at most 0.009.
Values may be sent and summed in bfloat16 or wider, within the bound.
A program may use at most 64 MiB of HBM per device.

```python
import math
import jax
import jax.numpy as jnp
import numpy as np
from jax import lax

D = 2048
CONV = 1024
FF = 1024
KTAPS = 3
TOPK = 2
TOKENS = 4096
ROWS = 128
EXPERTS = 32
CAP = 16
NDOCS = 4
DOC_MOST = 2048


def steps_of(key, shape, cuts, low, top_value):
    level = 1.0
    for axis_at, shards_of in cuts:
        heights = jax.random.uniform(jax.random.fold_in(jax.random.fold_in(key, 6), axis_at), (shards_of,), jnp.float32, low / len(cuts), top_value / len(cuts))
        level = level * jnp.repeat(jnp.exp(heights), shape[axis_at] // shards_of).reshape((-1,) + (1,) * (len(shape) - 1 - axis_at))
    return level


def length_profile(amount, total, most, skew):
    loads = [(1 << 20) // math.isqrt(standing ** skew) + 1 for standing in range(2, amount + 1)]
    surplus, given = total - most - (amount - 1), [1] * (amount - 1)
    while surplus > 0:
        free = [i for i in range(amount - 1) if given[i] < most]
        pool, left = sum([loads[i] for i in free]), surplus
        for i in free:
            more = min(most - given[i], max(1, left * loads[i] // pool), surplus)
            given[i] = given[i] + more
            surplus = surplus - more
    return np.array([most] + given)


def uneven(stream_key, number_of, total, most, slope):
    if number_of == 2:
        one = jax.random.randint(stream_key, (), max(1, total - most), min(most, total - 1) + 1)
        return jnp.stack([one, total - one])
    lengths = jnp.asarray(length_profile(number_of, total, most, slope), jnp.int32)
    twos = (number_of - 1) // 2
    giver, taker = lengths[1:1 + 2 * twos:2], lengths[2:2 + 2 * twos:2]
    slack = jnp.minimum(giver - 1, most - taker)
    shifted = jax.random.randint(jax.random.fold_in(stream_key, 1), (twos,), 0, 1 << 20) % (slack + 1)
    lengths = lengths.at[1:1 + 2 * twos:2].set(giver - shifted).at[2:2 + 2 * twos:2].set(taker + shifted)
    return lengths[jax.random.permutation(jax.random.fold_in(stream_key, 2), number_of)]


def routed_block(rng, own, number, rows, number_of, top, reach, slope):
    ranking = jax.random.permutation(rng, number_of)
    heavy_load, common = portions_of(number_of, rows * top, reach, slope, True), portions_of(number_of, rows * top, reach, slope, False)
    places = jnp.arange(number_of)

    def named(lengths, offset_by):
        used = int((lengths > 0).sum())
        fixed = max(1, used // 4)
        shifted = fixed + (places - fixed + offset_by * (used - fixed)) % max(1, number_of - fixed)
        return jnp.zeros((number_of,), jnp.int32).at[ranking[jnp.where(places < fixed, places, shifted)]].set(jnp.asarray(lengths, jnp.int32))

    lengths = jnp.where(number % 4 == 0, named(heavy_load, number // 4), named(common, number - number // 4 - 1))
    mixed = jax.random.permutation(jax.random.fold_in(own, 3), number_of)
    source_of, taker = mixed[0:number_of // 2 * 2:2], mixed[1:number_of // 2 * 2:2]
    slack = jnp.minimum(lengths[source_of] - 1, reach - lengths[taker]) // 2
    slack = jnp.where((source_of == ranking[0]) | (taker == ranking[0]) | (lengths[taker] == 0), 0, jnp.maximum(slack, 0))
    shifted = jax.random.randint(jax.random.fold_in(own, 4), (number_of // 2,), 0, 1 << 20) % (slack + 1)
    lengths = lengths.at[source_of].add(-shifted).at[taker].add(shifted)
    members = jnp.searchsorted(jnp.cumsum(lengths), jnp.arange(rows * top), side="right").astype(jnp.int32)
    table = members.reshape(top, rows).T
    table = table[jax.random.permutation(jax.random.fold_in(own, 1), rows)]
    offset_by = jax.random.randint(jax.random.fold_in(own, 2), (rows, 1), 0, top)
    return jnp.take_along_axis(table, (jnp.arange(top)[None, :] + offset_by) % top, axis=1)


def portions_of(amount, total, limit, skew, full):
    portions = [(1 << 20) // math.isqrt(rank ** skew) + 1 for rank in range(1, amount + 1)]
    largest = limit if full else min(limit, max(-(-total // amount), total * portions[0] // sum(portions)))
    least = 1 if total - largest >= amount - 1 else 0
    counts, rest = [largest] + [least] * (amount - 1), total - largest - least * (amount - 1)
    while rest > 0:
        free = [i for i in range(1, amount) if counts[i] < largest] or [i for i in range(1, amount) if counts[i] < limit]
        whole, budget = sum([portions[i] for i in free]), rest
        for i in free:
            extra = min(limit - counts[i], max(1, budget * portions[i] // whole), rest)
            counts[i] = counts[i] + extra
            rest = rest - extra
    return np.array(counts)


def gaussian(rng, dims, scale, reach, pieces=(), kind=jnp.bfloat16):
    result = jax.random.normal(rng, dims, jnp.float32) * scale
    if len(pieces) > 0:
        result = steps_of(rng, dims, pieces, -0.22, 0.18) * result
    return jnp.clip(result, min=-reach, max=reach).astype(kind)


def setup_inputs(seed: int = 0) -> dict:
    splits = jax.random.split(jax.random.key(seed), 14)
    conv_input = gaussian(splits[0], (TOKENS, CONV), 1.0, 6.0, ((0, 8), (1, 4)))
    gate_inner = gaussian(splits[1], (TOKENS, CONV), 1.0, 6.0, ((0, 8), (1, 4)))
    gate_outer = gaussian(splits[2], (TOKENS, CONV), 1.0, 6.0, ((0, 8), (1, 4)))
    conv_taps = gaussian(splits[3], (KTAPS, CONV), KTAPS ** -0.5, 3.5, ((1, 4),))
    doc_ids = jnp.searchsorted(jnp.cumsum(uneven(splits[4], NDOCS, TOKENS, DOC_MOST, 0)), jnp.arange(TOKENS), side="right").astype(jnp.int32)
    residual_in = gaussian(splits[5], (TOKENS, D), 1.0, 6.0, ((0, 32),))
    out_proj = gaussian(splits[6], (CONV, D), CONV ** -0.5, 0.1875)
    norm_gain = jnp.clip(1.0 + 0.18 * jax.random.normal(splits[7], (D,), jnp.float32), 0.1, 1.9)
    expert_ids_keys = jax.random.split(jax.random.fold_in(splits[8], 1), TOKENS // ROWS)
    expert_ids_turns = jax.random.permutation(jax.random.fold_in(splits[8], 3), TOKENS // ROWS)
    expert_ids = jax.vmap(lambda own, number: routed_block(jax.random.fold_in(splits[8], 2), own, number, ROWS, EXPERTS, TOPK, CAP, 1))(expert_ids_keys, expert_ids_turns).reshape((TOKENS, TOPK))
    expert_weights = jnp.clip(0.2 + 0.8 * jax.random.uniform(splits[9], (TOKENS, TOPK), jnp.float32) ** steps_of(splits[9], (TOKENS, TOPK), ((0, 32),), -0.2, 0.2), 0.2, 1.0)
    gate_proj = gaussian(splits[10], (EXPERTS, D, FF), D ** -0.5, 0.125, ((0, 32),))
    up_proj = gaussian(splits[11], (EXPERTS, D, FF), D ** -0.5, 0.125, ((0, 32),))
    down_proj = gaussian(splits[12], (EXPERTS, FF, D), FF ** -0.5, 0.1875, ((0, 32),))
    return {"conv_input": conv_input, "gate_inner": gate_inner, "gate_outer": gate_outer, "conv_taps": conv_taps, "doc_ids": doc_ids, "residual_in": residual_in, "out_proj": out_proj, "norm_gain": norm_gain, "expert_ids": expert_ids, "expert_weights": expert_weights, "gate_proj": gate_proj, "up_proj": up_proj, "down_proj": down_proj}


def expert_rows(arrived, gate_weight, up_weight, down_weight):
    gate_value = jnp.dot(arrived, gate_weight, preferred_element_type=jnp.float32)
    up_value = jnp.dot(arrived, up_weight, preferred_element_type=jnp.float32)
    hidden = (jax.nn.silu(gate_value) * up_value).astype(jnp.bfloat16)
    return jnp.dot(hidden, down_weight, preferred_element_type=jnp.float32).astype(jnp.bfloat16)

def reference(conv_input, gate_inner, gate_outer, conv_taps, doc_ids, residual_in, out_proj, norm_gain, expert_ids, expert_weights, gate_proj, up_proj, down_proj):
    inner_prod = conv_input.astype(jnp.float32) * gate_inner.astype(jnp.float32)
    tap_values = conv_taps.astype(jnp.float32)
    channels = inner_prod.shape[1]
    one_rows = jnp.concatenate([jnp.zeros((1, channels), jnp.float32), inner_prod[:-1]], axis=0)
    two_rows = jnp.concatenate([jnp.zeros((2, channels), jnp.float32), inner_prod[:-2]], axis=0)
    one_docs = jnp.concatenate([jnp.full((1,), -1, jnp.int32), doc_ids[:-1]], axis=0)
    two_docs = jnp.concatenate([jnp.full((2,), -1, jnp.int32), doc_ids[:-2]], axis=0)
    one_back = jnp.where((one_docs == doc_ids)[:, None], one_rows, 0.0)
    two_back = jnp.where((two_docs == doc_ids)[:, None], two_rows, 0.0)
    mixed_rows = tap_values[2] * inner_prod + tap_values[1] * one_back + tap_values[0] * two_back
    conv_out = (gate_outer.astype(jnp.float32) * mixed_rows).astype(jnp.bfloat16)
    mix = jnp.dot(conv_out, out_proj, preferred_element_type=jnp.float32).astype(jnp.bfloat16)
    carried = residual_in.astype(jnp.float32) + mix.astype(jnp.float32)
    normed = (carried * lax.rsqrt(lax.optimization_barrier(jnp.mean(carried * carried, axis=1, keepdims=True)) + 1e-06) * norm_gain).astype(jnp.bfloat16)
    choose = expert_ids.shape[1]
    blocks = TOKENS // ROWS
    block_ids = expert_ids.reshape(blocks, ROWS * choose)
    onehot = (block_ids[:, :, None] == jnp.arange(EXPERTS, dtype=jnp.int32)[None, None, :]).astype(jnp.int32)
    slot_rank = lax.optimization_barrier(jnp.sum((jnp.cumsum(onehot, axis=1) - 1) * onehot, axis=2))
    block_index = jnp.arange(blocks, dtype=jnp.int32)[:, None]
    target = (block_ids * (blocks * CAP) + block_index * CAP + slot_rank).reshape(-1).astype(jnp.int32)
    sources = jnp.repeat(normed, choose, axis=0)
    buffer = jnp.zeros((EXPERTS * blocks * CAP, D), jnp.bfloat16).at[target].set(sources)
    buffer = buffer.reshape(EXPERTS, blocks * CAP, D)

    def serve(operands):
        return expert_rows(operands[0], operands[1], operands[2], operands[3])
    results = lax.map(serve, (buffer, gate_proj, up_proj, down_proj))
    picked = results.reshape(-1, D)[target].reshape(TOKENS, choose, D).astype(jnp.float32)
    combined = carried + lax.optimization_barrier(jnp.sum(expert_weights[:, :, None] * picked, axis=1))
    return combined.astype(jnp.bfloat16)
```

```python
import functools

import jax
import jax.numpy as jnp
from jax import lax
from jax.experimental import pallas as pl
from jax.experimental.pallas import tpu as pltpu
from jax.sharding import PartitionSpec as P

MESH = pl.DeviceIdType.MESH


def layer_kernel(
    sp_count, tp_count, cap, pieces,
    x_ref, meta_ref, carried_ref, gate_hbm, up_hbm, down_hbm,
    out_ref,
    gate_w, up_w, down_w, meta_far, x_far, slots, arrived, hidden, served, back, part_out, part_in,
    w_sem, meta_sem, dense_send, dense_recv, part_send, part_recv, go_send, go_recv, ret_send, ret_recv,
):
    sp = lax.axis_index("sp")
    tp = lax.axis_index("tp")
    half = sp_count // 2
    group = half * tp_count
    base = lax.div(sp, half) * half
    mine = (sp - base) * tp_count + tp
    far = (lax.rem(sp + half, sp_count), tp)
    rows, width = x_ref.shape
    step = width // pieces
    ff = gate_w.shape[1]
    tile = 256
    slot_count = group * cap

    def where(member):
        return (base + lax.div(member, tp_count), lax.rem(member, tp_count))

    def peer(i):
        odd = lax.rem(i, 2)
        shift = group // 2 + (1 - 2 * odd) * lax.div(i + 1, 2)
        return lax.rem(mine + shift, group)

    loads = [
        pltpu.make_async_copy(source.at[0], target, w_sem.at[n])
        for n, (source, target) in enumerate(((gate_hbm, gate_w), (up_hbm, up_w), (down_hbm, down_w)))
    ]
    for load in loads:
        load.start()

    barrier = pltpu.get_barrier_semaphore()
    pl.semaphore_signal(barrier, inc=1, device_id=far, device_id_type=MESH)

    @pl.loop(0, group - 1)
    def _(i):
        pl.semaphore_signal(barrier, inc=1, device_id=where(peer(i)), device_id_type=MESH)

    pl.semaphore_wait(barrier, group)

    def dense_copy(c):
        return pltpu.make_async_remote_copy(
            src_ref=x_ref.at[:, pl.ds(c * step, step)], dst_ref=x_far.at[c],
            send_sem=dense_send.at[c], recv_sem=dense_recv.at[c], device_id=far, device_id_type=MESH,
        )

    def part_copy(c):
        return pltpu.make_async_remote_copy(
            src_ref=part_out.at[c], dst_ref=part_in.at[c],
            send_sem=part_send.at[c], recv_sem=part_recv.at[c], device_id=far, device_id_type=MESH,
        )

    def exchange(source, target, send, recv, p, c, other, landing):
        return pltpu.make_async_remote_copy(
            src_ref=source.at[p, c, other], dst_ref=target.at[p, c, landing],
            send_sem=send.at[p, c, other], recv_sem=recv.at[p, c, landing],
            device_id=where(other), device_id_type=MESH,
        )

    def send_all(source, target, send, recv, p, c):
        @pl.loop(0, group - 1)
        def _(i):
            exchange(source, target, send, recv, p, c, peer(i), mine).start()

        target[p, c, pl.ds(mine, 1)] = source[p, c, pl.ds(mine, 1)]

    def wait_all(source, target, send, recv, p, c):
        @pl.loop(0, group - 1)
        def _(i):
            other = peer(i)
            exchange(source, target, send, recv, p, c, other, other).wait_recv()

    def wait_sent(source, target, send, recv):
        for p in range(2):
            @pl.loop(0, pieces)
            def _(c):
                @pl.loop(0, group - 1)
                def _(i):
                    other = peer(i)
                    exchange(source, target, send, recv, p, c, other, other).wait_send()

    go = (slots, arrived, go_send, go_recv)
    ret = (served, back, ret_send, ret_recv)

    meta_copy = pltpu.make_async_remote_copy(
        src_ref=meta_ref, dst_ref=meta_far, send_sem=meta_sem.at[0], recv_sem=meta_sem.at[1],
        device_id=far, device_id_type=MESH,
    )
    meta_copy.start()

    def matches(meta):
        first = base * tp_count * cap
        ids = (lax.broadcasted_iota(jnp.int32, (slot_count, rows), 0) + first).astype(jnp.float32)
        choices = meta.shape[0] // 2
        return [(meta[k : k + 1, :] == ids, meta[choices + k : choices + k + 1, :]) for k in range(choices)]

    def placing(meta):
        total = jnp.zeros((slot_count, rows), jnp.float32)
        for hit, _ in matches(meta):
            total = total + jnp.where(hit, 1.0, 0.0)
        return total.astype(jnp.bfloat16)

    def weighing(meta):
        total = jnp.zeros((slot_count, rows), jnp.float32)
        for hit, weight in matches(meta):
            total = total + jnp.where(hit, weight, 0.0)
        total = total.T
        high = total.astype(jnp.bfloat16)
        return high, (total - high.astype(jnp.float32)).astype(jnp.bfloat16)

    def fill(p, c, place, block):
        picked = jnp.dot(place, block, preferred_element_type=jnp.float32).astype(jnp.bfloat16)
        slots[p, c] = picked.reshape(group, cap, step)
        send_all(*go, p, c)

    place = placing(meta_ref[...])
    for c in range(pieces):
        dense_copy(c).start()
        fill(0, c, place, x_ref[:, c * step : (c + 1) * step])

    meta_copy.wait()
    place = placing(meta_far[...])
    for c in range(pieces):
        dense_copy(c).wait_recv()
        fill(1, c, place, x_far[c])

    for p in range(2):
        for c in range(pieces):
            wait_all(*go, p, c)
        if p == 0:
            loads[0].wait()
            loads[1].wait()

        @pl.loop(0, ff // tile)
        def _(f):
            columns = pl.ds(pl.multiple_of(f * tile, tile), tile)
            gate_value = jnp.zeros((slot_count, tile), jnp.float32)
            up_value = jnp.zeros((slot_count, tile), jnp.float32)
            for c in range(pieces):
                piece = arrived[p, c].reshape(slot_count, step)
                lines = pl.ds(c * step, step)
                gate_value += jnp.dot(piece, gate_w[lines, columns], preferred_element_type=jnp.float32)
                up_value += jnp.dot(piece, up_w[lines, columns], preferred_element_type=jnp.float32)
            silu = gate_value * (1.0 / (1.0 + jnp.exp(-gate_value)))
            hidden[:, columns] = (silu * up_value).astype(jnp.bfloat16)

        if p == 0:
            loads[2].wait()

        for c in range(pieces):
            value = jnp.dot(
                hidden[...], down_w[:, c * step : (c + 1) * step], preferred_element_type=jnp.float32
            ).astype(jnp.bfloat16)
            served[p, c] = value.reshape(group, cap, step)
            send_all(*ret, p, c)

    def weighted(p, c, high, low):
        got = back[p, c].reshape(slot_count, step)
        return jnp.dot(high, got, preferred_element_type=jnp.float32) + jnp.dot(
            low, got, preferred_element_type=jnp.float32
        )

    high, low = weighing(meta_far[...])
    for c in range(pieces):
        wait_all(*ret, 1, c)
        part_out[c] = weighted(1, c, high, low).astype(jnp.bfloat16)
        part_copy(c).start()
    high, low = weighing(meta_ref[...])
    for c in range(pieces):
        wait_all(*ret, 0, c)
        total = carried_ref[:, c * step : (c + 1) * step] + weighted(0, c, high, low)
        part_copy(c).wait_recv()
        out_ref[:, c * step : (c + 1) * step] = (total + part_in[c].astype(jnp.float32)).astype(jnp.bfloat16)

    for c in range(pieces):
        dense_copy(c).wait_send()
        part_copy(c).wait_send()
    wait_sent(*go)
    wait_sent(*ret)


def run_layer(normed, meta, carried, gate_proj, up_proj, down_proj, cap, pieces=4):
    sp_count, tp_count = lax.axis_size("sp"), lax.axis_size("tp")
    rows, width = normed.shape
    ff = gate_proj.shape[2]
    group = sp_count // 2 * tp_count
    step = width // pieces
    slot_shape = (2, pieces, group, cap, step)
    dma = pltpu.SemaphoreType.DMA
    vmem = pl.BlockSpec(memory_space=pltpu.VMEM)
    hbm = pl.BlockSpec(memory_space=pl.ANY)
    return pl.pallas_call(
        functools.partial(layer_kernel, sp_count, tp_count, cap, pieces),
        out_shape=jax.ShapeDtypeStruct((rows, width), jnp.bfloat16),
        in_specs=[vmem, vmem, vmem, hbm, hbm, hbm],
        out_specs=vmem,
        scratch_shapes=[
            pltpu.VMEM((width, ff), jnp.bfloat16),
            pltpu.VMEM((width, ff), jnp.bfloat16),
            pltpu.VMEM((ff, width), jnp.bfloat16),
            pltpu.VMEM(meta.shape, jnp.float32),
            pltpu.VMEM((pieces, rows, step), jnp.bfloat16),
            pltpu.VMEM(slot_shape, jnp.bfloat16),
            pltpu.VMEM(slot_shape, jnp.bfloat16),
            pltpu.VMEM((group * cap, ff), jnp.bfloat16),
            pltpu.VMEM(slot_shape, jnp.bfloat16),
            pltpu.VMEM(slot_shape, jnp.bfloat16),
            pltpu.VMEM((pieces, rows, step), jnp.bfloat16),
            pltpu.VMEM((pieces, rows, step), jnp.bfloat16),
            dma((3,)),
            dma((2,)),
            dma((pieces,)),
            dma((pieces,)),
            dma((pieces,)),
            dma((pieces,)),
            dma((2, pieces, group)),
            dma((2, pieces, group)),
            dma((2, pieces, group)),
            dma((2, pieces, group)),
        ],
        compiler_params=pltpu.CompilerParams(
            collective_id=0, has_side_effects=True, vmem_limit_bytes=48 * 1024 * 1024
        ),
    )(normed, meta, carried, gate_proj, up_proj, down_proj)


def from_behind(block, axis, distance):
    devices = range(lax.axis_size(axis))
    route = [(i - distance, i) for i in devices if i - distance in devices]
    return lax.ppermute(block, axis, route)


def expert_rows(arrived, gate_weight, up_weight, down_weight):
    gate_value = jnp.dot(arrived, gate_weight, preferred_element_type=jnp.float32)
    up_value = jnp.dot(arrived, up_weight, preferred_element_type=jnp.float32)
    hidden = (jax.nn.silu(gate_value) * up_value).astype(jnp.bfloat16)
    return jnp.dot(hidden, down_weight, preferred_element_type=jnp.float32).astype(jnp.bfloat16)


def on_device(
    conv_input,
    gate_inner,
    gate_outer,
    conv_taps,
    doc_ids,
    residual_in,
    out_proj,
    norm_gain,
    expert_ids,
    expert_weights,
    gate_proj,
    up_proj,
    down_proj,
):
    inner_prod = conv_input.astype(jnp.float32) * gate_inner.astype(jnp.float32)
    earlier, earlier_docs = from_behind((inner_prod[-2:], doc_ids[-2:]), "sp", 1)
    padded = jnp.concatenate([earlier, inner_prod], axis=0)
    padded_docs = jnp.concatenate([earlier_docs, doc_ids], axis=0)
    length = inner_prod.shape[0]
    tap_values = conv_taps.astype(jnp.float32)
    one_back = jnp.where(
        (padded_docs[1 : length + 1] == doc_ids)[:, None], padded[1 : length + 1], 0.0
    )
    two_back = jnp.where((padded_docs[:length] == doc_ids)[:, None], padded[:length], 0.0)
    mixed_rows = tap_values[2] * inner_prod + tap_values[1] * one_back + tap_values[0] * two_back
    conv_out = (gate_outer.astype(jnp.float32) * mixed_rows).astype(jnp.bfloat16)
    row_count = residual_in.shape[0]
    regrouped = lax.all_to_all(conv_out, "tp", split_axis=0, concat_axis=1, tiled=True)
    mix = jnp.dot(regrouped, out_proj, preferred_element_type=jnp.float32).astype(jnp.bfloat16)
    carried = residual_in.astype(jnp.float32) + mix.astype(jnp.float32)
    normed = (
        carried * lax.rsqrt(jnp.mean(carried * carried, axis=1, keepdims=True) + 1e-06) * norm_gain
    ).astype(jnp.bfloat16)
    model_width = normed.shape[1]
    choose = expert_ids.shape[1]
    sp_count = lax.axis_size("sp")
    tp_count = lax.axis_size("tp")
    experts_total = sp_count * tp_count
    capacity = 2 * row_count * choose // experts_total
    flat_ids = expert_ids.reshape(-1)
    onehot = (flat_ids[:, None] == jnp.arange(experts_total, dtype=jnp.int32)[None, :]).astype(
        jnp.int32
    )
    slot_rank = jnp.sum((jnp.cumsum(onehot, axis=0) - 1) * onehot, axis=1)
    target = flat_ids * capacity + slot_rank
    if capacity % 16 == 0 and sp_count % 2 == 0:
        places = target.reshape(row_count, choose).astype(jnp.float32)
        meta = jnp.concatenate([places.T, expert_weights.T], axis=0)
        return run_layer(normed, meta, carried, gate_proj, up_proj, down_proj, capacity)
    sources = jnp.repeat(normed, choose, axis=0)
    outgoing = (
        jnp.zeros((experts_total * capacity, model_width), jnp.bfloat16).at[target].set(sources)
    )
    gate_weight = gate_proj[0]
    up_weight = up_proj[0]
    down_weight = down_proj[0]
    arrived = lax.all_to_all(
        outgoing.reshape(experts_total, capacity, model_width),
        ("sp", "tp"),
        split_axis=0,
        concat_axis=0,
        tiled=True,
    )
    item_count = arrived.shape[1]
    flat_rows = arrived.reshape(-1, model_width)
    result = expert_rows(flat_rows, gate_weight, up_weight, down_weight)
    result = result.reshape(experts_total, item_count, model_width)
    returned = lax.all_to_all(result, ("sp", "tp"), split_axis=0, concat_axis=0, tiled=True)
    picked = (
        returned.reshape(-1, model_width)[target]
        .reshape(row_count, choose, model_width)
        .astype(jnp.float32)
    )
    combined = carried + jnp.sum(expert_weights[:, :, None] * picked, axis=1)
    return combined.astype(jnp.bfloat16)


def solution(mesh):
    in_specs = (
        P("sp", "tp"),
        P("sp", "tp"),
        P("sp", "tp"),
        P(None, "tp"),
        P("sp"),
        P(("sp", "tp"), None),
        P(),
        P(),
        P(("sp", "tp"), None),
        P(("sp", "tp"), None),
        P(("sp", "tp"), None, None),
        P(("sp", "tp"), None, None),
        P(("sp", "tp"), None, None),
    )
    out_specs = P(("sp", "tp"), None)
    return jax.shard_map(
        on_device, mesh=mesh, in_specs=in_specs, out_specs=out_specs, check_vma=False
    )
```

```python
import functools

import jax
import jax.numpy as jnp
from jax import lax
from jax.experimental import pallas as pl
from jax.experimental.pallas import tpu as pltpu
from jax.sharding import PartitionSpec as P

MESH = pl.DeviceIdType.MESH


def layer_kernel(
    sp_count, tp_count, cap, pieces,
    conv_ref, inner_ref, outer_ref, taps_ref, docs_ref, residual_ref, gain_ref,
    meta_ref, gate_hbm, up_hbm, down_hbm, proj_hbm,
    out_ref,
    x_ref, carried_ref, proj_w, padded, padded_docs, tail, tail_in, conv_out, conv_in,
    gate_w, up_w, down_w, meta_far, x_far, slots, arrived, hidden, served, back, part_out, part_in,
    w_sem, tail_sem, conv_send, conv_recv, meta_sem, dense_send, dense_recv, part_send, part_recv, go_send, go_recv, ret_send, ret_recv,
):
    sp = lax.axis_index("sp")
    tp = lax.axis_index("tp")
    half = sp_count // 2
    group = half * tp_count
    base = lax.div(sp, half) * half
    mine = (sp - base) * tp_count + tp
    far = (lax.rem(sp + half, sp_count), tp)
    rows, width = x_ref.shape
    step = width // pieces
    ff = gate_w.shape[1]
    tile = 256
    slot_count = group * cap

    def where(member):
        return (base + lax.div(member, tp_count), lax.rem(member, tp_count))

    def peer(i):
        odd = lax.rem(i, 2)
        shift = group // 2 + (1 - 2 * odd) * lax.div(i + 1, 2)
        return lax.rem(mine + shift, group)

    pairs = ((gate_hbm.at[0], gate_w), (up_hbm.at[0], up_w), (down_hbm.at[0], down_w), (proj_hbm, proj_w))
    loads = [
        pltpu.make_async_copy(source, target, w_sem.at[n])
        for n, (source, target) in enumerate(pairs)
    ]
    for load in loads[3:] + loads[:3]:
        load.start()

    barrier = pltpu.get_barrier_semaphore()
    pl.semaphore_signal(barrier, inc=1, device_id=far, device_id_type=MESH)

    @pl.loop(0, group - 1)
    def _(i):
        pl.semaphore_signal(barrier, inc=1, device_id=where(peer(i)), device_id_type=MESH)

    after = (lax.rem(sp + 1, sp_count), tp)
    before = (lax.rem(sp + sp_count - 1, sp_count), tp)
    for neighbour in (after, before):
        pl.semaphore_signal(barrier, inc=1, device_id=neighbour, device_id_type=MESH)

    length, channels = conv_ref.shape
    lanes = docs_ref.shape[1]
    edge = tail.shape[0]
    padded[edge:, :] = conv_ref[...].astype(jnp.float32) * inner_ref[...].astype(jnp.float32)
    padded_docs[edge:, :] = docs_ref[...]
    tail[:, :channels] = padded[length:, :]
    tail[:, channels:] = padded_docs[length:, :]
    pl.semaphore_wait(barrier, group + 2)

    tail_copy = pltpu.make_async_remote_copy(
        src_ref=tail, dst_ref=tail_in, send_sem=tail_sem.at[0], recv_sem=tail_sem.at[1],
        device_id=after, device_id_type=MESH,
    )
    tail_copy.start()
    tail_copy.wait()
    padded[:edge, :] = tail_in[:, :channels]
    padded_docs[:edge, :] = jnp.where(sp == 0, -1.0, tail_in[:, channels:])
    docs = docs_ref[...]
    same_one = padded_docs[edge - 1 : edge - 1 + length, :] == docs
    same_two = padded_docs[edge - 2 : edge - 2 + length, :] == docs
    taps = taps_ref[...].astype(jnp.float32)
    for k in range(channels // lanes):
        at = slice(k * lanes, (k + 1) * lanes)
        one_back = jnp.where(same_one, padded[edge - 1 : edge - 1 + length, at], 0.0)
        two_back = jnp.where(same_two, padded[edge - 2 : edge - 2 + length, at], 0.0)
        mixed = taps[2:3, at] * padded[edge:, at] + taps[1:2, at] * one_back + taps[0:1, at] * two_back
        gated = (outer_ref[:, at].astype(jnp.float32) * mixed).astype(jnp.bfloat16)
        conv_out[:, :, at] = gated.reshape(tp_count, rows, lanes)

    def conv_copy(other, landing):
        return pltpu.make_async_remote_copy(
            src_ref=conv_out.at[other], dst_ref=conv_in.at[landing],
            send_sem=conv_send.at[other], recv_sem=conv_recv.at[landing],
            device_id=(sp, other), device_id_type=MESH,
        )

    others = [lax.rem(tp + j, tp_count) for j in range(1, tp_count)]
    for other in others:
        conv_copy(other, tp).start()
    conv_in[pl.ds(tp, 1)] = conv_out[pl.ds(tp, 1)]
    loads[3].wait()
    for other in others:
        conv_copy(other, other).wait_recv()
    for c in range(pieces):
        at = slice(c * step, (c + 1) * step)
        mix = jnp.zeros((rows, step), jnp.float32)
        for j in range(tp_count):
            lines = slice(j * channels, (j + 1) * channels)
            mix += jnp.dot(conv_in[j], proj_w[lines, at], preferred_element_type=jnp.float32)
        carried_ref[:, at] = residual_ref[:, at].astype(jnp.float32) + mix.astype(jnp.bfloat16).astype(jnp.float32)
    carried = carried_ref[...]
    scale = lax.rsqrt(jnp.mean(carried * carried, axis=1, keepdims=True) + 1e-06)
    x_ref[...] = (carried * scale * gain_ref[...]).astype(jnp.bfloat16)

    def dense_copy(c):
        return pltpu.make_async_remote_copy(
            src_ref=x_ref.at[:, pl.ds(c * step, step)], dst_ref=x_far.at[c],
            send_sem=dense_send.at[c], recv_sem=dense_recv.at[c], device_id=far, device_id_type=MESH,
        )

    def part_copy(c):
        return pltpu.make_async_remote_copy(
            src_ref=part_out.at[c], dst_ref=part_in.at[c],
            send_sem=part_send.at[c], recv_sem=part_recv.at[c], device_id=far, device_id_type=MESH,
        )

    def exchange(source, target, send, recv, p, c, other, landing):
        return pltpu.make_async_remote_copy(
            src_ref=source.at[p, c, other], dst_ref=target.at[p, c, landing],
            send_sem=send.at[p, c, other], recv_sem=recv.at[p, c, landing],
            device_id=where(other), device_id_type=MESH,
        )

    def send_all(source, target, send, recv, p, c):
        @pl.loop(0, group - 1)
        def _(i):
            exchange(source, target, send, recv, p, c, peer(i), mine).start()

        target[p, c, pl.ds(mine, 1)] = source[p, c, pl.ds(mine, 1)]

    def wait_all(source, target, send, recv, p, c):
        @pl.loop(0, group - 1)
        def _(i):
            other = peer(i)
            exchange(source, target, send, recv, p, c, other, other).wait_recv()

    def wait_sent(source, target, send, recv):
        for p in range(2):
            @pl.loop(0, pieces)
            def _(c):
                @pl.loop(0, group - 1)
                def _(i):
                    other = peer(i)
                    exchange(source, target, send, recv, p, c, other, other).wait_send()

    go = (slots, arrived, go_send, go_recv)
    ret = (served, back, ret_send, ret_recv)

    meta_copy = pltpu.make_async_remote_copy(
        src_ref=meta_ref, dst_ref=meta_far, send_sem=meta_sem.at[0], recv_sem=meta_sem.at[1],
        device_id=far, device_id_type=MESH,
    )
    meta_copy.start()

    def matches(meta):
        first = base * tp_count * cap
        ids = (lax.broadcasted_iota(jnp.int32, (slot_count, rows), 0) + first).astype(jnp.float32)
        choices = meta.shape[0] // 2
        return [(meta[k : k + 1, :] == ids, meta[choices + k : choices + k + 1, :]) for k in range(choices)]

    def placing(meta):
        total = jnp.zeros((slot_count, rows), jnp.float32)
        for hit, _ in matches(meta):
            total = total + jnp.where(hit, 1.0, 0.0)
        return total.astype(jnp.bfloat16)

    def weighing(meta):
        total = jnp.zeros((slot_count, rows), jnp.float32)
        for hit, weight in matches(meta):
            total = total + jnp.where(hit, weight, 0.0)
        total = total.T
        high = total.astype(jnp.bfloat16)
        return high, (total - high.astype(jnp.float32)).astype(jnp.bfloat16)

    def fill(p, c, place, block):
        picked = jnp.dot(place, block, preferred_element_type=jnp.float32).astype(jnp.bfloat16)
        slots[p, c] = picked.reshape(group, cap, step)
        send_all(*go, p, c)

    place = placing(meta_ref[...])
    for c in range(pieces):
        dense_copy(c).start()
        fill(0, c, place, x_ref[:, c * step : (c + 1) * step])

    meta_copy.wait()
    place = placing(meta_far[...])
    for c in range(pieces):
        dense_copy(c).wait_recv()
        fill(1, c, place, x_far[c])

    for p in range(2):
        for c in range(pieces):
            wait_all(*go, p, c)
        if p == 0:
            loads[0].wait()
            loads[1].wait()

        @pl.loop(0, ff // tile)
        def _(f):
            columns = pl.ds(pl.multiple_of(f * tile, tile), tile)
            gate_value = jnp.zeros((slot_count, tile), jnp.float32)
            up_value = jnp.zeros((slot_count, tile), jnp.float32)
            for c in range(pieces):
                piece = arrived[p, c].reshape(slot_count, step)
                lines = pl.ds(c * step, step)
                gate_value += jnp.dot(piece, gate_w[lines, columns], preferred_element_type=jnp.float32)
                up_value += jnp.dot(piece, up_w[lines, columns], preferred_element_type=jnp.float32)
            silu = gate_value * (1.0 / (1.0 + jnp.exp(-gate_value)))
            hidden[:, columns] = (silu * up_value).astype(jnp.bfloat16)

        if p == 0:
            loads[2].wait()

        for c in range(pieces):
            value = jnp.dot(
                hidden[...], down_w[:, c * step : (c + 1) * step], preferred_element_type=jnp.float32
            ).astype(jnp.bfloat16)
            served[p, c] = value.reshape(group, cap, step)
            send_all(*ret, p, c)

    def weighted(p, c, high, low):
        got = back[p, c].reshape(slot_count, step)
        return jnp.dot(high, got, preferred_element_type=jnp.float32) + jnp.dot(
            low, got, preferred_element_type=jnp.float32
        )

    high, low = weighing(meta_far[...])
    for c in range(pieces):
        wait_all(*ret, 1, c)
        part_out[c] = weighted(1, c, high, low).astype(jnp.bfloat16)
        part_copy(c).start()
    high, low = weighing(meta_ref[...])
    for c in range(pieces):
        wait_all(*ret, 0, c)
        total = carried_ref[:, c * step : (c + 1) * step] + weighted(0, c, high, low)
        part_copy(c).wait_recv()
        out_ref[:, c * step : (c + 1) * step] = (total + part_in[c].astype(jnp.float32)).astype(jnp.bfloat16)

    for other in others:
        conv_copy(other, other).wait_send()
    for c in range(pieces):
        dense_copy(c).wait_send()
        part_copy(c).wait_send()
    wait_sent(*go)
    wait_sent(*ret)


def run_layer(front, meta, gate_proj, up_proj, down_proj, out_proj, cap, pieces=4):
    sp_count, tp_count = lax.axis_size("sp"), lax.axis_size("tp")
    length, channels = front[0].shape
    lanes = front[4].shape[1]
    rows, width = front[5].shape
    edge = 8
    ff = gate_proj.shape[2]
    group = sp_count // 2 * tp_count
    step = width // pieces
    slot_shape = (2, pieces, group, cap, step)
    dma = pltpu.SemaphoreType.DMA
    vmem = pl.BlockSpec(memory_space=pltpu.VMEM)
    hbm = pl.BlockSpec(memory_space=pl.ANY)
    return pl.pallas_call(
        functools.partial(layer_kernel, sp_count, tp_count, cap, pieces),
        out_shape=jax.ShapeDtypeStruct((rows, width), jnp.bfloat16),
        in_specs=[vmem] * 8 + [hbm] * 4,
        out_specs=vmem,
        scratch_shapes=[
            pltpu.VMEM((rows, width), jnp.bfloat16),
            pltpu.VMEM((rows, width), jnp.float32),
            pltpu.VMEM(out_proj.shape, jnp.bfloat16),
            pltpu.VMEM((edge + length, channels), jnp.float32),
            pltpu.VMEM((edge + length, lanes), jnp.float32),
            pltpu.VMEM((edge, channels + lanes), jnp.float32),
            pltpu.VMEM((edge, channels + lanes), jnp.float32),
            pltpu.VMEM((tp_count, rows, channels), jnp.bfloat16),
            pltpu.VMEM((tp_count, rows, channels), jnp.bfloat16),
            pltpu.VMEM((width, ff), jnp.bfloat16),
            pltpu.VMEM((width, ff), jnp.bfloat16),
            pltpu.VMEM((ff, width), jnp.bfloat16),
            pltpu.VMEM(meta.shape, jnp.float32),
            pltpu.VMEM((pieces, rows, step), jnp.bfloat16),
            pltpu.VMEM(slot_shape, jnp.bfloat16),
            pltpu.VMEM(slot_shape, jnp.bfloat16),
            pltpu.VMEM((group * cap, ff), jnp.bfloat16),
            pltpu.VMEM(slot_shape, jnp.bfloat16),
            pltpu.VMEM(slot_shape, jnp.bfloat16),
            pltpu.VMEM((pieces, rows, step), jnp.bfloat16),
            pltpu.VMEM((pieces, rows, step), jnp.bfloat16),
            dma((4,)),
            dma((2,)),
            dma((tp_count,)),
            dma((tp_count,)),
            dma((2,)),
            dma((pieces,)),
            dma((pieces,)),
            dma((pieces,)),
            dma((pieces,)),
            dma((2, pieces, group)),
            dma((2, pieces, group)),
            dma((2, pieces, group)),
            dma((2, pieces, group)),
        ],
        compiler_params=pltpu.CompilerParams(
            collective_id=0, has_side_effects=True, vmem_limit_bytes=48 * 1024 * 1024
        ),
    )(*front, meta, gate_proj, up_proj, down_proj, out_proj)


def from_behind(block, axis, distance):
    devices = range(lax.axis_size(axis))
    route = [(i - distance, i) for i in devices if i - distance in devices]
    return lax.ppermute(block, axis, route)


def expert_rows(arrived, gate_weight, up_weight, down_weight):
    gate_value = jnp.dot(arrived, gate_weight, preferred_element_type=jnp.float32)
    up_value = jnp.dot(arrived, up_weight, preferred_element_type=jnp.float32)
    hidden = (jax.nn.silu(gate_value) * up_value).astype(jnp.bfloat16)
    return jnp.dot(hidden, down_weight, preferred_element_type=jnp.float32).astype(jnp.bfloat16)


def on_device(
    conv_input,
    gate_inner,
    gate_outer,
    conv_taps,
    doc_ids,
    residual_in,
    out_proj,
    norm_gain,
    expert_ids,
    expert_weights,
    gate_proj,
    up_proj,
    down_proj,
):
    inner_prod = conv_input.astype(jnp.float32) * gate_inner.astype(jnp.float32)
    earlier, earlier_docs = from_behind((inner_prod[-2:], doc_ids[-2:]), "sp", 1)
    padded = jnp.concatenate([earlier, inner_prod], axis=0)
    padded_docs = jnp.concatenate([earlier_docs, doc_ids], axis=0)
    length = inner_prod.shape[0]
    tap_values = conv_taps.astype(jnp.float32)
    one_back = jnp.where(
        (padded_docs[1 : length + 1] == doc_ids)[:, None], padded[1 : length + 1], 0.0
    )
    two_back = jnp.where((padded_docs[:length] == doc_ids)[:, None], padded[:length], 0.0)
    mixed_rows = tap_values[2] * inner_prod + tap_values[1] * one_back + tap_values[0] * two_back
    conv_out = (gate_outer.astype(jnp.float32) * mixed_rows).astype(jnp.bfloat16)
    row_count = residual_in.shape[0]
    regrouped = lax.all_to_all(conv_out, "tp", split_axis=0, concat_axis=1, tiled=True)
    mix = jnp.dot(regrouped, out_proj, preferred_element_type=jnp.float32).astype(jnp.bfloat16)
    carried = residual_in.astype(jnp.float32) + mix.astype(jnp.float32)
    normed = (
        carried * lax.rsqrt(jnp.mean(carried * carried, axis=1, keepdims=True) + 1e-06) * norm_gain
    ).astype(jnp.bfloat16)
    model_width = normed.shape[1]
    choose = expert_ids.shape[1]
    sp_count = lax.axis_size("sp")
    tp_count = lax.axis_size("tp")
    experts_total = sp_count * tp_count
    capacity = 2 * row_count * choose // experts_total
    flat_ids = expert_ids.reshape(-1)
    onehot = (flat_ids[:, None] == jnp.arange(experts_total, dtype=jnp.int32)[None, :]).astype(
        jnp.int32
    )
    slot_rank = jnp.sum((jnp.cumsum(onehot, axis=0) - 1) * onehot, axis=1)
    target = flat_ids * capacity + slot_rank
    if capacity % 16 == 0 and sp_count % 2 == 0:
        places = target.reshape(row_count, choose).astype(jnp.float32)
        meta = jnp.concatenate([places.T, expert_weights.T], axis=0)
        docs = jnp.broadcast_to(doc_ids.astype(jnp.float32)[:, None], (doc_ids.shape[0], 128))
        front = (conv_input, gate_inner, gate_outer, conv_taps, docs, residual_in, norm_gain[None, :])
        return run_layer(front, meta, gate_proj, up_proj, down_proj, out_proj, capacity)
    sources = jnp.repeat(normed, choose, axis=0)
    outgoing = (
        jnp.zeros((experts_total * capacity, model_width), jnp.bfloat16).at[target].set(sources)
    )
    gate_weight = gate_proj[0]
    up_weight = up_proj[0]
    down_weight = down_proj[0]
    arrived = lax.all_to_all(
        outgoing.reshape(experts_total, capacity, model_width),
        ("sp", "tp"),
        split_axis=0,
        concat_axis=0,
        tiled=True,
    )
    item_count = arrived.shape[1]
    flat_rows = arrived.reshape(-1, model_width)
    result = expert_rows(flat_rows, gate_weight, up_weight, down_weight)
    result = result.reshape(experts_total, item_count, model_width)
    returned = lax.all_to_all(result, ("sp", "tp"), split_axis=0, concat_axis=0, tiled=True)
    picked = (
        returned.reshape(-1, model_width)[target]
        .reshape(row_count, choose, model_width)
        .astype(jnp.float32)
    )
    combined = carried + jnp.sum(expert_weights[:, :, None] * picked, axis=1)
    return combined.astype(jnp.bfloat16)


def solution(mesh):
    in_specs = (
        P("sp", "tp"),
        P("sp", "tp"),
        P("sp", "tp"),
        P(None, "tp"),
        P("sp"),
        P(("sp", "tp"), None),
        P(),
        P(),
        P(("sp", "tp"), None),
        P(("sp", "tp"), None),
        P(("sp", "tp"), None, None),
        P(("sp", "tp"), None, None),
        P(("sp", "tp"), None, None),
    )
    out_specs = P(("sp", "tp"), None)
    return jax.shard_map(
        on_device, mesh=mesh, in_specs=in_specs, out_specs=out_specs, check_vma=False
    )
```

```python
import functools

import jax
import jax.numpy as jnp
from jax import lax
from jax.experimental import pallas as pl
from jax.experimental.pallas import tpu as pltpu
from jax.sharding import PartitionSpec as P

MESH = pl.DeviceIdType.MESH


def layer_kernel(
    sp_count, tp_count, cap, pieces,
    conv_ref, inner_ref, outer_ref, taps_ref, docs_ref, residual_ref, gain_ref,
    meta_ref, gate_hbm, up_hbm, down_hbm, proj_hbm,
    out_ref,
    x_ref, carried_ref, proj_w, padded, padded_docs, tail, tail_in, conv_out, conv_in,
    gate_w, up_w, down_w, meta_far, x_far, slots, arrived, hidden, served, back, part_out, part_in,
    w_sem, tail_sem, conv_send, conv_recv, meta_sem, dense_send, dense_recv, part_send, part_recv, go_send, go_recv, ret_send, ret_recv,
):
    sp = lax.axis_index("sp")
    tp = lax.axis_index("tp")
    half = sp_count // 2
    group = half * tp_count
    base = lax.div(sp, half) * half
    mine = (sp - base) * tp_count + tp
    far = (lax.rem(sp + half, sp_count), tp)
    rows, width = x_ref.shape
    step = width // pieces
    ff = gate_w.shape[1]
    tile = 256
    slot_count = group * cap

    def where(member):
        return (base + lax.div(member, tp_count), lax.rem(member, tp_count))

    def peer(i):
        odd = lax.rem(i, 2)
        shift = group // 2 + (1 - 2 * odd) * lax.div(i + 1, 2)
        return lax.rem(mine + shift, group)

    pairs = ((gate_hbm.at[0], gate_w), (up_hbm.at[0], up_w), (down_hbm.at[0], down_w), (proj_hbm, proj_w))
    loads = [
        pltpu.make_async_copy(source, target, w_sem.at[n])
        for n, (source, target) in enumerate(pairs)
    ]
    for load in loads[3:] + loads[:3]:
        load.start()

    barrier = pltpu.get_barrier_semaphore()
    pl.semaphore_signal(barrier, inc=1, device_id=far, device_id_type=MESH)

    @pl.loop(0, group - 1)
    def _(i):
        pl.semaphore_signal(barrier, inc=1, device_id=where(peer(i)), device_id_type=MESH)

    after = (lax.rem(sp + 1, sp_count), tp)
    before = (lax.rem(sp + sp_count - 1, sp_count), tp)
    for neighbour in (after, before):
        pl.semaphore_signal(barrier, inc=1, device_id=neighbour, device_id_type=MESH)

    length, channels = conv_ref.shape
    lanes = docs_ref.shape[1]
    edge = tail.shape[0]
    padded[edge:, :] = conv_ref[...].astype(jnp.float32) * inner_ref[...].astype(jnp.float32)
    padded_docs[edge:, :] = docs_ref[...]
    tail[:, :channels] = padded[length:, :]
    tail[:, channels:] = padded_docs[length:, :]
    pl.semaphore_wait(barrier, group + 2)

    tail_copy = pltpu.make_async_remote_copy(
        src_ref=tail, dst_ref=tail_in, send_sem=tail_sem.at[0], recv_sem=tail_sem.at[1],
        device_id=after, device_id_type=MESH,
    )
    tail_copy.start()
    tail_copy.wait()
    padded[:edge, :] = tail_in[:, :channels]
    padded_docs[:edge, :] = jnp.where(sp == 0, -1.0, tail_in[:, channels:])
    docs = docs_ref[...]
    same_one = padded_docs[edge - 1 : edge - 1 + length, :] == docs
    same_two = padded_docs[edge - 2 : edge - 2 + length, :] == docs
    taps = taps_ref[...].astype(jnp.float32)
    for k in range(channels // lanes):
        at = slice(k * lanes, (k + 1) * lanes)
        one_back = jnp.where(same_one, padded[edge - 1 : edge - 1 + length, at], 0.0)
        two_back = jnp.where(same_two, padded[edge - 2 : edge - 2 + length, at], 0.0)
        mixed = taps[2:3, at] * padded[edge:, at] + taps[1:2, at] * one_back + taps[0:1, at] * two_back
        gated = (outer_ref[:, at].astype(jnp.float32) * mixed).astype(jnp.bfloat16)
        conv_out[:, :, at] = gated.reshape(tp_count, rows, lanes)

    def conv_copy(other, landing):
        return pltpu.make_async_remote_copy(
            src_ref=conv_out.at[other], dst_ref=conv_in.at[landing],
            send_sem=conv_send.at[other], recv_sem=conv_recv.at[landing],
            device_id=(sp, other), device_id_type=MESH,
        )

    others = [lax.rem(tp + j, tp_count) for j in range(1, tp_count)]
    for other in others:
        conv_copy(other, tp).start()
    conv_in[pl.ds(tp, 1)] = conv_out[pl.ds(tp, 1)]
    loads[3].wait()
    for other in others:
        conv_copy(other, other).wait_recv()
    for c in range(pieces):
        at = slice(c * step, (c + 1) * step)
        mix = jnp.zeros((rows, step), jnp.float32)
        for j in range(tp_count):
            lines = slice(j * channels, (j + 1) * channels)
            mix += jnp.dot(conv_in[j], proj_w[lines, at], preferred_element_type=jnp.float32)
        carried_ref[:, at] = residual_ref[:, at].astype(jnp.float32) + mix.astype(jnp.bfloat16).astype(jnp.float32)
    carried = carried_ref[...]
    scale = lax.rsqrt(jnp.mean(carried * carried, axis=1, keepdims=True) + 1e-06)
    x_ref[...] = (carried * scale * gain_ref[...]).astype(jnp.bfloat16)

    def dense_copy(c):
        return pltpu.make_async_remote_copy(
            src_ref=x_ref.at[:, pl.ds(c * step, step)], dst_ref=x_far.at[c],
            send_sem=dense_send.at[c], recv_sem=dense_recv.at[c], device_id=far, device_id_type=MESH,
        )

    def part_copy(c):
        return pltpu.make_async_remote_copy(
            src_ref=part_out.at[c], dst_ref=part_in.at[c],
            send_sem=part_send.at[c], recv_sem=part_recv.at[c], device_id=far, device_id_type=MESH,
        )

    def exchange(source, target, send, recv, p, c, other, landing):
        return pltpu.make_async_remote_copy(
            src_ref=source.at[p, c, other], dst_ref=target.at[p, c, landing],
            send_sem=send.at[p, c, other], recv_sem=recv.at[p, c, landing],
            device_id=where(other), device_id_type=MESH,
        )

    def send_all(source, target, send, recv, p, c):
        @pl.loop(0, group - 1)
        def _(i):
            exchange(source, target, send, recv, p, c, peer(i), mine).start()

        target[p, c, pl.ds(mine, 1)] = source[p, c, pl.ds(mine, 1)]

    def wait_all(source, target, send, recv, p, c):
        @pl.loop(0, group - 1)
        def _(i):
            other = peer(i)
            exchange(source, target, send, recv, p, c, other, other).wait_recv()

    def wait_sent(source, target, send, recv):
        for p in range(2):
            @pl.loop(0, pieces)
            def _(c):
                @pl.loop(0, group - 1)
                def _(i):
                    other = peer(i)
                    exchange(source, target, send, recv, p, c, other, other).wait_send()

    go = (slots, arrived, go_send, go_recv)
    ret = (served, back, ret_send, ret_recv)

    meta_copy = pltpu.make_async_remote_copy(
        src_ref=meta_ref, dst_ref=meta_far, send_sem=meta_sem.at[0], recv_sem=meta_sem.at[1],
        device_id=far, device_id_type=MESH,
    )
    meta_copy.start()

    def matches(meta):
        first = base * tp_count * cap
        ids = (lax.broadcasted_iota(jnp.int32, (slot_count, rows), 0) + first).astype(jnp.float32)
        choices = meta.shape[0] // 2
        return [(meta[k : k + 1, :] == ids, meta[choices + k : choices + k + 1, :]) for k in range(choices)]

    def placing(meta):
        total = jnp.zeros((slot_count, rows), jnp.float32)
        for hit, _ in matches(meta):
            total = total + jnp.where(hit, 1.0, 0.0)
        return total.astype(jnp.bfloat16)

    def weighing(meta):
        total = jnp.zeros((slot_count, rows), jnp.float32)
        for hit, weight in matches(meta):
            total = total + jnp.where(hit, weight, 0.0)
        total = total.T
        high = total.astype(jnp.bfloat16)
        return high, (total - high.astype(jnp.float32)).astype(jnp.bfloat16)

    def fill(p, c, place, block):
        picked = jnp.dot(place, block, preferred_element_type=jnp.float32).astype(jnp.bfloat16)
        slots[p, c] = picked.reshape(group, cap, step)
        send_all(*go, p, c)

    place = placing(meta_ref[...])
    for c in range(pieces):
        dense_copy(c).start()
        fill(0, c, place, x_ref[:, c * step : (c + 1) * step])

    meta_copy.wait()
    place = placing(meta_far[...])
    for c in range(pieces):
        dense_copy(c).wait_recv()
        fill(1, c, place, x_far[c])

    for p in range(2):
        for c in range(pieces):
            wait_all(*go, p, c)
        if p == 0:
            loads[0].wait()
            loads[1].wait()

        @pl.loop(0, ff // tile)
        def _(f):
            columns = pl.ds(pl.multiple_of(f * tile, tile), tile)
            gate_value = jnp.zeros((slot_count, tile), jnp.float32)
            up_value = jnp.zeros((slot_count, tile), jnp.float32)
            for c in range(pieces):
                piece = arrived[p, c].reshape(slot_count, step)
                lines = pl.ds(c * step, step)
                gate_value += jnp.dot(piece, gate_w[lines, columns], preferred_element_type=jnp.float32)
                up_value += jnp.dot(piece, up_w[lines, columns], preferred_element_type=jnp.float32)
            silu = gate_value * (1.0 / (1.0 + jnp.exp(-gate_value)))
            hidden[:, columns] = (silu * up_value).astype(jnp.bfloat16)

        if p == 0:
            loads[2].wait()

        for c in range(pieces):
            value = jnp.dot(
                hidden[...], down_w[:, c * step : (c + 1) * step], preferred_element_type=jnp.float32
            ).astype(jnp.bfloat16)
            served[p, c] = value.reshape(group, cap, step)
            send_all(*ret, p, c)

    def weighted(p, c, high, low):
        got = back[p, c].reshape(slot_count, step)
        return jnp.dot(high, got, preferred_element_type=jnp.float32) + jnp.dot(
            low, got, preferred_element_type=jnp.float32
        )

    high, low = weighing(meta_far[...])
    for c in range(pieces):
        wait_all(*ret, 1, c)
        part_out[c] = weighted(1, c, high, low).astype(jnp.bfloat16)
        part_copy(c).start()
    high, low = weighing(meta_ref[...])
    for c in range(pieces):
        wait_all(*ret, 0, c)
        total = carried_ref[:, c * step : (c + 1) * step] + weighted(0, c, high, low)
        part_copy(c).wait_recv()
        out_ref[:, c * step : (c + 1) * step] = (total + part_in[c].astype(jnp.float32)).astype(jnp.bfloat16)

    for other in others:
        conv_copy(other, other).wait_send()
    for c in range(pieces):
        dense_copy(c).wait_send()
        part_copy(c).wait_send()
    wait_sent(*go)
    wait_sent(*ret)


def run_layer(front, meta, gate_proj, up_proj, down_proj, out_proj, cap, pieces=2):
    sp_count, tp_count = lax.axis_size("sp"), lax.axis_size("tp")
    length, channels = front[0].shape
    lanes = front[4].shape[1]
    rows, width = front[5].shape
    edge = 8
    ff = gate_proj.shape[2]
    group = sp_count // 2 * tp_count
    step = width // pieces
    slot_shape = (2, pieces, group, cap, step)
    dma = pltpu.SemaphoreType.DMA
    vmem = pl.BlockSpec(memory_space=pltpu.VMEM)
    hbm = pl.BlockSpec(memory_space=pl.ANY)
    return pl.pallas_call(
        functools.partial(layer_kernel, sp_count, tp_count, cap, pieces),
        out_shape=jax.ShapeDtypeStruct((rows, width), jnp.bfloat16),
        in_specs=[vmem] * 8 + [hbm] * 4,
        out_specs=vmem,
        scratch_shapes=[
            pltpu.VMEM((rows, width), jnp.bfloat16),
            pltpu.VMEM((rows, width), jnp.float32),
            pltpu.VMEM(out_proj.shape, jnp.bfloat16),
            pltpu.VMEM((edge + length, channels), jnp.float32),
            pltpu.VMEM((edge + length, lanes), jnp.float32),
            pltpu.VMEM((edge, channels + lanes), jnp.float32),
            pltpu.VMEM((edge, channels + lanes), jnp.float32),
            pltpu.VMEM((tp_count, rows, channels), jnp.bfloat16),
            pltpu.VMEM((tp_count, rows, channels), jnp.bfloat16),
            pltpu.VMEM((width, ff), jnp.bfloat16),
            pltpu.VMEM((width, ff), jnp.bfloat16),
            pltpu.VMEM((ff, width), jnp.bfloat16),
            pltpu.VMEM(meta.shape, jnp.float32),
            pltpu.VMEM((pieces, rows, step), jnp.bfloat16),
            pltpu.VMEM(slot_shape, jnp.bfloat16),
            pltpu.VMEM(slot_shape, jnp.bfloat16),
            pltpu.VMEM((group * cap, ff), jnp.bfloat16),
            pltpu.VMEM(slot_shape, jnp.bfloat16),
            pltpu.VMEM(slot_shape, jnp.bfloat16),
            pltpu.VMEM((pieces, rows, step), jnp.bfloat16),
            pltpu.VMEM((pieces, rows, step), jnp.bfloat16),
            dma((4,)),
            dma((2,)),
            dma((tp_count,)),
            dma((tp_count,)),
            dma((2,)),
            dma((pieces,)),
            dma((pieces,)),
            dma((pieces,)),
            dma((pieces,)),
            dma((2, pieces, group)),
            dma((2, pieces, group)),
            dma((2, pieces, group)),
            dma((2, pieces, group)),
        ],
        compiler_params=pltpu.CompilerParams(
            collective_id=0, has_side_effects=True, vmem_limit_bytes=48 * 1024 * 1024
        ),
    )(*front, meta, gate_proj, up_proj, down_proj, out_proj)


def from_behind(block, axis, distance):
    devices = range(lax.axis_size(axis))
    route = [(i - distance, i) for i in devices if i - distance in devices]
    return lax.ppermute(block, axis, route)


def expert_rows(arrived, gate_weight, up_weight, down_weight):
    gate_value = jnp.dot(arrived, gate_weight, preferred_element_type=jnp.float32)
    up_value = jnp.dot(arrived, up_weight, preferred_element_type=jnp.float32)
    hidden = (jax.nn.silu(gate_value) * up_value).astype(jnp.bfloat16)
    return jnp.dot(hidden, down_weight, preferred_element_type=jnp.float32).astype(jnp.bfloat16)


def on_device(
    conv_input,
    gate_inner,
    gate_outer,
    conv_taps,
    doc_ids,
    residual_in,
    out_proj,
    norm_gain,
    expert_ids,
    expert_weights,
    gate_proj,
    up_proj,
    down_proj,
):
    inner_prod = conv_input.astype(jnp.float32) * gate_inner.astype(jnp.float32)
    earlier, earlier_docs = from_behind((inner_prod[-2:], doc_ids[-2:]), "sp", 1)
    padded = jnp.concatenate([earlier, inner_prod], axis=0)
    padded_docs = jnp.concatenate([earlier_docs, doc_ids], axis=0)
    length = inner_prod.shape[0]
    tap_values = conv_taps.astype(jnp.float32)
    one_back = jnp.where(
        (padded_docs[1 : length + 1] == doc_ids)[:, None], padded[1 : length + 1], 0.0
    )
    two_back = jnp.where((padded_docs[:length] == doc_ids)[:, None], padded[:length], 0.0)
    mixed_rows = tap_values[2] * inner_prod + tap_values[1] * one_back + tap_values[0] * two_back
    conv_out = (gate_outer.astype(jnp.float32) * mixed_rows).astype(jnp.bfloat16)
    row_count = residual_in.shape[0]
    regrouped = lax.all_to_all(conv_out, "tp", split_axis=0, concat_axis=1, tiled=True)
    mix = jnp.dot(regrouped, out_proj, preferred_element_type=jnp.float32).astype(jnp.bfloat16)
    carried = residual_in.astype(jnp.float32) + mix.astype(jnp.float32)
    normed = (
        carried * lax.rsqrt(jnp.mean(carried * carried, axis=1, keepdims=True) + 1e-06) * norm_gain
    ).astype(jnp.bfloat16)
    model_width = normed.shape[1]
    choose = expert_ids.shape[1]
    sp_count = lax.axis_size("sp")
    tp_count = lax.axis_size("tp")
    experts_total = sp_count * tp_count
    capacity = 2 * row_count * choose // experts_total
    flat_ids = expert_ids.reshape(-1)
    onehot = (flat_ids[:, None] == jnp.arange(experts_total, dtype=jnp.int32)[None, :]).astype(
        jnp.int32
    )
    slot_rank = jnp.sum((jnp.cumsum(onehot, axis=0) - 1) * onehot, axis=1)
    target = flat_ids * capacity + slot_rank
    if capacity % 16 == 0 and sp_count % 2 == 0:
        places = target.reshape(row_count, choose).astype(jnp.float32)
        meta = jnp.concatenate([places.T, expert_weights.T], axis=0)
        docs = jnp.broadcast_to(doc_ids.astype(jnp.float32)[:, None], (doc_ids.shape[0], 128))
        front = (conv_input, gate_inner, gate_outer, conv_taps, docs, residual_in, norm_gain[None, :])
        return run_layer(front, meta, gate_proj, up_proj, down_proj, out_proj, capacity)
    sources = jnp.repeat(normed, choose, axis=0)
    outgoing = (
        jnp.zeros((experts_total * capacity, model_width), jnp.bfloat16).at[target].set(sources)
    )
    gate_weight = gate_proj[0]
    up_weight = up_proj[0]
    down_weight = down_proj[0]
    arrived = lax.all_to_all(
        outgoing.reshape(experts_total, capacity, model_width),
        ("sp", "tp"),
        split_axis=0,
        concat_axis=0,
        tiled=True,
    )
    item_count = arrived.shape[1]
    flat_rows = arrived.reshape(-1, model_width)
    result = expert_rows(flat_rows, gate_weight, up_weight, down_weight)
    result = result.reshape(experts_total, item_count, model_width)
    returned = lax.all_to_all(result, ("sp", "tp"), split_axis=0, concat_axis=0, tiled=True)
    picked = (
        returned.reshape(-1, model_width)[target]
        .reshape(row_count, choose, model_width)
        .astype(jnp.float32)
    )
    combined = carried + jnp.sum(expert_weights[:, :, None] * picked, axis=1)
    return combined.astype(jnp.bfloat16)


def solution(mesh):
    in_specs = (
        P("sp", "tp"),
        P("sp", "tp"),
        P("sp", "tp"),
        P(None, "tp"),
        P("sp"),
        P(("sp", "tp"), None),
        P(),
        P(),
        P(("sp", "tp"), None),
        P(("sp", "tp"), None),
        P(("sp", "tp"), None, None),
        P(("sp", "tp"), None, None),
        P(("sp", "tp"), None, None),
    )
    out_specs = P(("sp", "tp"), None)
    return jax.shard_map(
        on_device, mesh=mesh, in_specs=in_specs, out_specs=out_specs, check_vma=False
    )
```
